32 devices in a mesh: sp: 8 (over z, x), tp: 4 (over y, core).
Axes of the slice: x: 2, y: 2, z: 4, core: 2. Of those that a mesh axis runs over, the one named last changes fastest.
Arguments:
- moe_in: bfloat16 [1536, 2048], P('sp'), may hold values from -6 to 6
- out_grad: bfloat16 [1536, 2048], P('sp'), may hold values from -6 to 6
- expert_ids: int32 [1536, 2], P('sp'), may hold values from 0 to 7, all different within a row; in each aligned block of 192 rows (0 to 191, 192 to 383, ...) at most 96 rows name the same one
- route_weights: float32 [1536, 2], P('sp'), may hold values from 0.1 to 0.9
- gate_proj: bfloat16 [8, 2048, 2048], P('sp', None, 'tp'), may hold values from -0.125 to 0.125
- up_proj: bfloat16 [8, 2048, 2048], P('sp', None, 'tp'), may hold values from -0.125 to 0.125
- down_proj: bfloat16 [8, 2048, 2048], P('sp', 'tp'), may hold values from -0.125 to 0.125
- out_proj: bfloat16 [2048, 2048], P('tp'), may hold values from -0.125 to 0.125
- conv_out: bfloat16 [1536, 2048], P('sp'), may hold values from -8 to 8
- conv_taps: float32 [31, 2048], P(None, 'tp'), may hold values from -1 to 1
Outputs:
- gate_grad: float32 [8, 2048, 2048], P('sp', None, 'tp')
- up_grad: float32 [8, 2048, 2048], P('sp', None, 'tp')
- down_grad: float32 [8, 2048, 2048], P('sp', 'tp')
- proj_grad: float32 [2048, 2048], P('sp', 'tp')
- input_grad: bfloat16 [1536, 2048], P('sp', 'tp')
The draws below stay inside these ranges and needn't reach their ends.
Inputs may be any that keep to these rules, and one draw needn't show every extreme that they name: `expert_ids`: each row names 2 different experts. Among the rows of one index of sp (aligned blocks of 192 rows), no expert is named by more than 96 rows, a bound that some block reaches.
All inputs are finite; a program needn't handle non-finite values.
Results may differ from the reference program's by a relative error of at most 0.019.
Values may be sent and summed in bfloat16 or wider, within the bound.
A program may use at most 64 MiB of HBM per device.

```python
import math
import jax
import jax.numpy as jnp
import numpy as np
from jax import lax

D = 2048
FFE = 2048
TOK_DEV = 192
TOP = 2
KSIZE = 31
EXPERTS = 8
TOKENS = 1536
CAP = 96
N_SP = 8
N_TP = 4


def with_spikes(values, own_key, source, target, shards_of, factor):
    owner, partner = [(jnp.arange(values.shape[axis_at]) // (values.shape[axis_at] // shards_of)).reshape([-1 if axis == axis_at else 1 for axis in range(values.ndim)]) for axis_at in (source, target)]
    chosen = jax.random.permutation(own_key, shards_of)[partner]
    strong = (owner == chosen) | (owner == (partner + shards_of // 2) % shards_of)
    return jnp.where(strong, factor * values, values)


def levels(own_key, shape, split, low, largest):
    gain = 1.0
    for dim, shards_of in split:
        steps = jax.random.uniform(jax.random.fold_in(jax.random.fold_in(own_key, 6), dim), (shards_of,), jnp.float32, low / len(split), largest / len(split))
        gain = gain * jnp.repeat(jnp.exp(steps), shape[dim] // shards_of).reshape((-1,) + (1,) * (len(shape) - 1 - dim))
    return gain


def shared_out(own_key, own, number, rows, number_of, top, most, skew):
    order = jax.random.permutation(own_key, number_of)
    heavy_load, usual = load_shares(number_of, rows * top, most, skew, True), load_shares(number_of, rows * top, most, skew, False)
    places = jnp.arange(number_of)

    def named(sizes, rotation):
        used = int((sizes > 0).sum())
        fixed = max(1, used // 4)
        passed = fixed + (places - fixed + rotation * (used - fixed)) % max(1, number_of - fixed)
        return jnp.zeros((number_of,), jnp.int32).at[order[jnp.where(places < fixed, places, passed)]].set(jnp.asarray(sizes, jnp.int32))

    sizes = jnp.where(number % 4 == 0, named(heavy_load, number // 4), named(usual, number - number // 4 - 1))
    mixed = jax.random.permutation(jax.random.fold_in(own, 3), number_of)
    giver, sink = mixed[0:number_of // 2 * 2:2], mixed[1:number_of // 2 * 2:2]
    margin = jnp.minimum(sizes[giver] - 1, most - sizes[sink]) // 2
    margin = jnp.where((giver == order[0]) | (sink == order[0]) | (sizes[sink] == 0), 0, jnp.maximum(margin, 0))
    passed = jax.random.randint(jax.random.fold_in(own, 4), (number_of // 2,), 0, 1 << 20) % (margin + 1)
    sizes = sizes.at[giver].add(-passed).at[sink].add(passed)
    labels = jnp.searchsorted(jnp.cumsum(sizes), jnp.arange(rows * top), side="right").astype(jnp.int32)
    grid = labels.reshape(top, rows).T
    grid = grid[jax.random.permutation(jax.random.fold_in(own, 1), rows)]
    rotation = jax.random.randint(jax.random.fold_in(own, 2), (rows, 1), 0, top)
    return jnp.take_along_axis(grid, (jnp.arange(top)[None, :] + rotation) % top, axis=1)


def load_shares(amount, total, reach, skew, full):
    portions = [(1 << 20) // math.isqrt(grade ** skew) + 1 for grade in range(1, amount + 1)]
    largest = reach if full else min(reach, max(-(-total // amount), total * portions[0] // sum(portions)))
    least = 1 if total - largest >= amount - 1 else 0
    counts, surplus = [largest] + [least] * (amount - 1), total - largest - least * (amount - 1)
    while surplus > 0:
        free = [i for i in range(1, amount) if counts[i] < largest] or [i for i in range(1, amount) if counts[i] < reach]
        pool, remaining = sum([portions[i] for i in free]), surplus
        for i in free:
            addition = min(reach - counts[i], max(1, remaining * portions[i] // pool), surplus)
            counts[i] = counts[i] + addition
            surplus = surplus - addition
    return np.array(counts)


def scatter_about(key, extent, scale, most, shards=(), held_as=jnp.bfloat16):
    loudness = levels(key, extent, shards, -0.22, 0.18) if shards else 1.0
    drawn = jax.random.normal(key, extent, jnp.float32) * scale * loudness
    return jnp.minimum(jnp.maximum(drawn, -most), most).astype(held_as)


def noise_with(key, dims, deviation, reach, pieces, heavy, kind=jnp.bfloat16):
    entries = deviation * jax.random.normal(key, dims, jnp.float32)
    if pieces:
        entries = entries * levels(key, dims, pieces, -0.22, 0.18)
    return jnp.clip(with_spikes(entries, jax.random.fold_in(key, 3), *heavy), -reach, reach).astype(kind)


def setup_inputs(seed: int = 0) -> dict:
    key_of = jax.random.split(jax.random.key(seed), 11)
    moe_in = scatter_about(key_of[0], (TOKENS, D), 1.0, 6.0, ((0, 8),))
    out_grad = noise_with(key_of[1], (TOKENS, D), 1.0, 6.0, ((0, 8),), (0, 1, 8, 2.0))
    expert_ids_keys = jax.random.split(jax.random.fold_in(key_of[2], 1), TOKENS // TOK_DEV)
    expert_ids_turns = jax.random.permutation(jax.random.fold_in(key_of[2], 3), TOKENS // TOK_DEV)
    expert_ids = jax.vmap(lambda own, number: shared_out(jax.random.fold_in(key_of[2], 2), own, number, TOK_DEV, EXPERTS, TOP, CAP, 2))(expert_ids_keys, expert_ids_turns).reshape((TOKENS, TOP))
    route_weights = jnp.clip(0.1 + 0.79999997 * jax.random.uniform(key_of[3], (TOKENS, TOP), jnp.float32) ** levels(key_of[3], (TOKENS, TOP), ((0, 8),), -0.2, 0.2), 0.1, 0.9)
    gate_proj = scatter_about(key_of[4], (EXPERTS, D, FFE), D ** -0.5, 0.125, ((0, 8), (2, 4)))
    up_proj = scatter_about(key_of[5], (EXPERTS, D, FFE), D ** -0.5, 0.125, ((0, 8), (2, 4)))
    down_proj = scatter_about(key_of[6], (EXPERTS, FFE, D), FFE ** -0.5, 0.125, ((0, 8), (1, 4)))
    out_proj = scatter_about(key_of[7], (D, D), D ** -0.5, 0.125, ((0, 4),))
    conv_out = scatter_about(key_of[8], (TOKENS, D), 1.5, 8.0, ((0, 8),))
    conv_taps = scatter_about(key_of[9], (KSIZE, D), KSIZE ** -0.5, 1.0, ((1, 4),), jnp.float32)
    return dict(moe_in=moe_in, out_grad=out_grad, expert_ids=expert_ids, route_weights=route_weights, gate_proj=gate_proj, up_proj=up_proj, down_proj=down_proj, out_proj=out_proj, conv_out=conv_out, conv_taps=conv_taps)


def dsilu(value):
    sig = jax.nn.sigmoid(value)
    return sig * (1.0 + value * (1.0 - sig))


def reference(moe_in, out_grad, expert_ids, route_weights, gate_proj, up_proj, down_proj, out_proj, conv_out, conv_taps):
    assigns = TOKENS * TOP
    per_expert = N_SP * CAP
    flat_e = expert_ids.reshape(-1).astype(jnp.int32)
    flat_t = (jnp.arange(assigns, dtype=jnp.int32) // TOP).astype(jnp.int32)
    flat_w = route_weights.reshape(-1)
    onehot = (flat_e[:, None] == jnp.arange(EXPERTS, dtype=jnp.int32)[None, :]).astype(jnp.int32)
    rank = jnp.sum((jnp.cumsum(onehot, axis=0) - onehot) * onehot, axis=1).astype(jnp.int32)
    dest = (flat_e * per_expert + rank).astype(jnp.int32)
    slot_tok = jnp.full((EXPERTS * per_expert,), TOKENS, jnp.int32).at[dest].set(flat_t).reshape(EXPERTS, per_expert)
    slot_w = jnp.zeros((EXPERTS * per_expert,), jnp.float32).at[dest].set(flat_w).reshape(EXPERTS, per_expert)
    x_pad = jnp.concatenate([moe_in, jnp.zeros((1, D), moe_in.dtype)], axis=0)
    g_pad = jnp.concatenate([out_grad, jnp.zeros((1, D), out_grad.dtype)], axis=0)
    width = FFE // N_TP

    def one_expert(args):
        tok, wts, w_gate, w_up, w_down = args
        rows_x = x_pad[tok]
        rows_g = (g_pad[tok].astype(jnp.float32) * wts[:, None]).astype(jnp.bfloat16)
        a_pre = jnp.dot(rows_x, w_gate, preferred_element_type=jnp.float32)
        b_pre = jnp.dot(rows_x, w_up, preferred_element_type=jnp.float32)
        hidden = (jax.nn.silu(a_pre) * b_pre).astype(jnp.bfloat16)
        d_down = jnp.dot(hidden.T, rows_g, preferred_element_type=jnp.float32)
        d_hidden = jnp.dot(rows_g, w_down.T, preferred_element_type=jnp.float32)
        d_a = (d_hidden * b_pre * dsilu(a_pre)).astype(jnp.bfloat16)
        d_b = (d_hidden * jax.nn.silu(a_pre)).astype(jnp.bfloat16)
        d_gate = jnp.dot(rows_x.T, d_a, preferred_element_type=jnp.float32)
        d_up = jnp.dot(rows_x.T, d_b, preferred_element_type=jnp.float32)
        total = jnp.zeros((per_expert, D), jnp.float32)
        for block in range(N_TP):
            low = block * width
            part = jnp.dot(d_a[:, low:low + width], w_gate[:, low:low + width].T, preferred_element_type=jnp.float32)
            part = part + jnp.dot(d_b[:, low:low + width], w_up[:, low:low + width].T, preferred_element_type=jnp.float32)
            total = total + part.astype(jnp.bfloat16).astype(jnp.float32)
        return d_gate, d_up, d_down, total.astype(jnp.bfloat16)

    gate_grad, up_grad, down_grad, row_grads = lax.map(one_expert, (slot_tok, slot_w, gate_proj, up_proj, down_proj))
    flat_rows = row_grads.reshape(EXPERTS * per_expert, D)
    routed = flat_rows[dest].astype(jnp.float32).reshape(TOKENS, TOP, D).sum(axis=1)
    mixed_grad = (out_grad.astype(jnp.float32) + routed).astype(jnp.bfloat16)
    conv32 = conv_out.astype(jnp.float32)
    act = jax.nn.silu(conv32).astype(jnp.bfloat16)
    proj_grad = jnp.dot(act.T, mixed_grad, preferred_element_type=jnp.float32)
    act_grad = jnp.dot(mixed_grad, out_proj.T, preferred_element_type=jnp.float32)
    conv_grad = act_grad * dsilu(conv32)
    extended = jnp.concatenate([conv_grad, jnp.zeros((KSIZE - 1, D), jnp.float32)], axis=0)
    result = jnp.zeros((TOKENS, D), jnp.float32)
    for tap in range(KSIZE):
        offset = KSIZE - 1 - tap
        result = result + conv_taps[tap][None, :] * extended[offset:offset + TOKENS]
    return gate_grad, up_grad, down_grad, proj_grad, result.astype(jnp.bfloat16)
```

```python
import functools

import jax
import jax.numpy as jnp
from jax import lax
from jax.experimental import pallas as pl
from jax.experimental.pallas import tpu as pltpu
from jax.sharding import PartitionSpec as P

MESH = pl.DeviceIdType.MESH


def dsilu(value):
    sig = jax.nn.sigmoid(value)
    return sig * (1.0 + value * (1.0 - sig))


def contract_rows(left, right):
    return lax.dot_general(
        left, right, (((0,), (0,)), ((), ())), preferred_element_type=jnp.float32
    )


def contract_cols(left, right):
    return lax.dot_general(
        left, right, (((1,), (1,)), ((), ())), preferred_element_type=jnp.float32
    )


def far_first(count):
    return sorted(range(1, count), key=lambda step: -min(step, count - step))


def peer_of(index, mask, count):
    other = index
    bit = 1
    while bit < count:
        if mask & bit:
            other = other + bit * (1 - 2 * lax.rem(index // bit, 2))
        bit *= 2
    return other


def iota(shape, dim):
    return lax.broadcasted_iota(jnp.int32, shape, dim)


def experts_kernel(
    ns, nt, cap, moe_in, out_grad, ids, weights, gate, up, down,
    o_x, o_g, o_hidden, o_da, o_db,
    x_all, g_all, w_gate, w_up, w_down, send_x, send_g, rows_x, rows_g,
    a_pre, b_pre, hidden, d_a, d_b, rank, route,
    load, asend, arecv, ysend, yrecv, dsend, drecv, store,
):
    sp, tp = lax.axis_index("sp"), lax.axis_index("tp")
    ny = nt // 2
    other_core = tp + 1 - 2 * lax.rem(tp, 2)
    tokens, model_width = moe_in.shape
    top = ids.shape[1]
    width = model_width // nt
    bf16, f32 = jnp.bfloat16, jnp.float32
    masks = list(range(1, ns))
    near, far = masks[: ns // 2 - 1], masks[ns // 2 - 1 :]
    sends, rows = (send_x, send_g), (rows_x, rows_g)

    loads = [
        pltpu.make_async_copy(src, dst, load.at[i])
        for i, (src, dst) in enumerate(
            ((moe_in, x_all), (out_grad, g_all), (gate, w_gate), (up, w_up), (down, w_down))
        )
    ]
    for copy in loads:
        copy.start()

    barrier = pltpu.get_barrier_semaphore()
    for mask in masks:
        pl.semaphore_signal(
            barrier, inc=1, device_id=(peer_of(sp, mask, ns), tp), device_id_type=MESH
        )
    for k in range(1, ny):
        pl.semaphore_signal(
            barrier, inc=1, device_id=(sp, lax.rem(tp + 2 * k, nt)), device_id_type=MESH
        )
    pl.semaphore_signal(barrier, inc=1, device_id=(sp, other_core), device_id_type=MESH)

    lane = iota((tokens, 128), 1)
    packed = jnp.zeros((tokens, 128), f32)
    for r in range(top):
        packed = jnp.where(lane == r, ids[:, r : r + 1].astype(f32), packed)
        packed = jnp.where(lane == top + r, weights[:, r : r + 1], packed)
    turned = packed.T
    count = rank.shape[0]
    expert = iota((count, tokens), 0).astype(f32)
    named = jnp.zeros((count, tokens), f32)
    weight = jnp.zeros((count, tokens), f32)
    for r in range(top):
        hit = turned[r : r + 1, :] == expert
        named = jnp.where(hit, 1.0, named)
        weight = jnp.where(hit, turned[top + r : top + r + 1, :], weight)
    earlier = (iota((tokens, tokens), 0) < iota((tokens, tokens), 1)).astype(f32).astype(bf16)
    place_of = jnp.dot(named.astype(bf16), earlier, preferred_element_type=f32)
    rank[...] = jnp.where(named > 0.0, place_of, -1.0)
    route[...] = weight

    def chosen_for(e):
        return rank[pl.ds(e, 1), :] == iota((cap, tokens), 0).astype(f32)

    def rows_of(kind, e, full):
        chosen = chosen_for(e)
        pick = chosen.astype(f32).astype(bf16)
        if full:
            source = (x_all, g_all)[kind][...]
        else:
            source = (x_all, g_all)[kind][:, pl.ds(pl.multiple_of(tp * width, 128), width)]
        value = jnp.dot(pick, source, preferred_element_type=f32)
        if kind == 1:
            slot = jnp.sum(jnp.where(chosen, route[pl.ds(e, 1), :], 0.0), axis=1, keepdims=True)
            value = value * slot
        return value.astype(bf16)

    def block(kind, src, part):
        return rows[kind].at[
            pl.ds(pl.multiple_of(src * cap, 16), cap),
            pl.ds(pl.multiple_of(part * width, 128), width),
        ]

    def across(kind, mask):
        dest = peer_of(sp, mask, ns)
        return pltpu.make_async_remote_copy(
            src_ref=sends[kind].at[mask],
            dst_ref=block(kind, sp, tp),
            send_sem=asend.at[kind, mask],
            recv_sem=arecv.at[kind, mask],
            device_id=(dest, tp),
            device_id_type=MESH,
        )

    def to_chip(kind, mask, k):
        src = peer_of(sp, mask, ns)
        return pltpu.make_async_remote_copy(
            src_ref=block(kind, src, tp),
            dst_ref=block(kind, src, tp),
            send_sem=ysend.at[kind, mask, k],
            recv_sem=yrecv.at[kind, mask, k],
            device_id=(sp, lax.rem(tp + 2 * k, nt)),
            device_id_type=MESH,
        )

    def to_core(kind, mask, k):
        src = peer_of(sp, mask, ns)
        part = lax.rem(tp - 2 * k + nt, nt)
        return pltpu.make_async_remote_copy(
            src_ref=block(kind, src, part),
            dst_ref=block(kind, src, part),
            send_sem=dsend.at[kind, mask, k],
            recv_sem=drecv.at[kind, mask, k],
            device_id=(sp, other_core),
            device_id_type=MESH,
        )

    loads[0].wait()
    pl.semaphore_wait(barrier, ns - 1 + ny - 1 + 1)
    waiting = None
    for kind in range(2):
        if kind == 1:
            loads[1].wait()
        for mask in masks:
            sends[kind][mask] = rows_of(kind, peer_of(sp, mask, ns), False)
            if waiting is not None:
                across(*waiting).start()
            waiting = (kind, mask)
    own = pl.ds(pl.multiple_of(sp * cap, 16), cap)
    rows_x[own, :] = rows_of(0, sp, True)
    across(*waiting).start()
    rows_g[own, :] = rows_of(1, sp, True)

    order = [(0, m) for m in near] + [(0, far[0])]
    for i, m in enumerate(far[1:]):
        order.append((0, m))
        if i < len(near):
            order.append((1, near[i]))
    order += [(1, m) for m in near[len(far) - 1 :]] + [(1, m) for m in far]
    lag = 2
    half = ns * cap // 2
    low = pl.multiple_of(sp // (ns // 2) * half, 16)
    high = pl.multiple_of((1 - sp // (ns // 2)) * half, 16)
    columns = w_gate.shape[1]
    piece = min(columns, 256)

    def first_stage(kind, mask):
        across(kind, mask).wait_recv()
        for k in range(1, ny):
            to_chip(kind, mask, k).start()
        to_core(kind, mask, 0).start()

    def second_stage(kind, mask):
        for k in range(1, ny):
            to_chip(kind, mask, k).wait_recv()
            to_core(kind, mask, k).start()

    def third_stage(kind, mask):
        for k in range(ny):
            to_core(kind, mask, k).wait_recv()

    def forward(start, part):
        cols = pl.ds(part * piece, piece)
        picked = pl.ds(start, half)
        x = rows_x[picked, :]
        a = jnp.dot(x, w_gate[:, cols], preferred_element_type=f32)
        b = jnp.dot(x, w_up[:, cols], preferred_element_type=f32)
        a_pre[picked, cols] = a
        b_pre[picked, cols] = b
        hidden[picked, cols] = (a * jax.nn.sigmoid(a) * b).astype(bf16)

    def backward(start, part):
        cols = pl.ds(part * piece, piece)
        picked = pl.ds(start, half)
        dh = lax.dot_general(
            rows_g[picked, :], w_down[cols, :], (((1,), (1,)), ((), ())),
            preferred_element_type=f32,
        )
        a, b = a_pre[picked, cols], b_pre[picked, cols]
        sig = jax.nn.sigmoid(a)
        d_a[picked, cols] = (dh * b * (sig * (1.0 + a * (1.0 - sig)))).astype(bf16)
        d_b[picked, cols] = (dh * (a * sig)).astype(bf16)

    parts = range(columns // piece)
    work = []
    seen = {0: 0, 1: 0}
    ready = []
    done_first = []

    def save(i, src, dst):
        return pltpu.make_async_copy(src, dst, store.at[i])

    saves = [
        save(0, rows_x, o_x), save(1, rows_g, o_g), save(2, hidden, o_hidden),
        save(3, d_a, o_da), save(4, d_b, o_db),
    ]
    loaded = [False]

    def weights_ready():
        if not loaded[0]:
            loaded[0] = True
            for copy in loads[2:]:
                copy.wait()

    started = set()

    def drain(limit):
        for _ in range(limit):
            if work:
                weights_ready()
                work.pop(0)()

    settled = {0: [], 1: []}

    def after_second(kind, mask):
        settled[kind].append(mask)
        group = settled[kind]
        if all(m in group for m in near) and (kind, "near") not in started:
            started.add((kind, "near"))
            for m in near:
                third_stage(kind, m)
            for part in parts:
                fn = forward if kind == 0 else backward
                work.append(functools.partial(fn, low, part))
        if all(m in group for m in far) and (kind, "far") not in started:
            started.add((kind, "far"))
            for m in far:
                third_stage(kind, m)
            saves[kind].start()
            for part in parts:
                fn = forward if kind == 0 else backward
                work.append(functools.partial(fn, high, part))

    for i, item in enumerate(order):
        first_stage(*item)
        if i >= lag:
            second_stage(*order[i - lag])
            after_second(*order[i - lag])
        if i >= len(order) // 2:
            drain(1)
    for item in order[-lag:]:
        second_stage(*item)
        after_second(*item)
    drain(len(work))
    for copy in saves[2:]:
        copy.start()
    for kind in range(2):
        for mask in masks:
            across(kind, mask).wait_send()
            for k in range(1, ny):
                to_chip(kind, mask, k).wait_send()
            for k in range(ny):
                to_core(kind, mask, k).wait_send()
    for copy in saves:
        copy.wait()


def experts(moe_in, out_grad, ids, weights, gate, up, down, ns, nt, cap):
    tokens, model_width = moe_in.shape
    columns = gate.shape[1]
    width = model_width // nt
    ny = nt // 2
    total = ns * cap
    bf16, f32 = jnp.bfloat16, jnp.float32
    any_spec = pl.BlockSpec(memory_space=pl.ANY)
    vmem = pl.BlockSpec(memory_space=pltpu.VMEM)
    dma = pltpu.SemaphoreType.DMA
    wide = jax.ShapeDtypeStruct((total, model_width), bf16)
    slim = jax.ShapeDtypeStruct((total, columns), bf16)
    return pl.pallas_call(
        functools.partial(experts_kernel, ns, nt, cap),
        out_shape=(wide, wide, slim, slim, slim),
        in_specs=[any_spec, any_spec, vmem, vmem, any_spec, any_spec, any_spec],
        out_specs=(any_spec,) * 5,
        scratch_shapes=[
            pltpu.VMEM((tokens, model_width), bf16),
            pltpu.VMEM((tokens, model_width), bf16),
            pltpu.VMEM(gate.shape, bf16),
            pltpu.VMEM(up.shape, bf16),
            pltpu.VMEM(down.shape, bf16),
            pltpu.VMEM((ns, cap, width), bf16),
            pltpu.VMEM((ns, cap, width), bf16),
            pltpu.VMEM((total, model_width), bf16),
            pltpu.VMEM((total, model_width), bf16),
            pltpu.VMEM((total, columns), f32),
            pltpu.VMEM((total, columns), f32),
            pltpu.VMEM((total, columns), bf16),
            pltpu.VMEM((total, columns), bf16),
            pltpu.VMEM((total, columns), bf16),
            pltpu.VMEM((max(ns, 8), tokens), f32),
            pltpu.VMEM((max(ns, 8), tokens), f32),
            dma((5,)),
            dma((2, ns)), dma((2, ns)),
            dma((2, ns, ny)), dma((2, ns, ny)), dma((2, ns, ny)), dma((2, ns, ny)),
            dma((5,)),
        ],
        compiler_params=pltpu.CompilerParams(collective_id=1, has_side_effects=True),
    )(moe_in, out_grad, ids, weights, gate, up, down)


def gather_kernel(ns, block, out, asend, arecv, fsend, frecv, local):
    sp, tp = lax.axis_index("sp"), lax.axis_index("tp")
    pair = sp + 1 - 2 * lax.rem(sp, 2)
    order = [2 * k for k in far_first(ns // 2)]

    barrier = pltpu.get_barrier_semaphore()
    for step in order:
        pl.semaphore_signal(
            barrier, inc=1, device_id=(lax.rem(sp + step, ns), tp), device_id_type=MESH
        )
    pl.semaphore_signal(barrier, inc=1, device_id=(pair, tp), device_id_type=MESH)
    pl.semaphore_wait(barrier, len(order) + 1)

    def along(step):
        return pltpu.make_async_remote_copy(
            src_ref=block,
            dst_ref=out.at[sp],
            send_sem=asend.at[step],
            recv_sem=arecv.at[step],
            device_id=(lax.rem(sp + step, ns), tp),
            device_id_type=MESH,
        )

    def to_pair(step):
        src = lax.rem(sp - step + ns, ns)
        return pltpu.make_async_remote_copy(
            src_ref=block if step == 0 else out.at[src],
            dst_ref=out.at[src],
            send_sem=fsend.at[step],
            recv_sem=frecv.at[step],
            device_id=(pair, tp),
            device_id_type=MESH,
        )

    for step in order:
        along(step).start()
    to_pair(0).start()
    keep = pltpu.make_async_copy(block, out.at[sp], local)
    keep.start()
    for step in order:
        along(step).wait_recv()
        to_pair(step).start()
    keep.wait()
    for step in order:
        along(step).wait_send()
    for step in [0] + order:
        to_pair(step).wait()


def gather_tokens(block, ns):
    any_spec = pl.BlockSpec(memory_space=pl.ANY)
    dma = pltpu.SemaphoreType.DMA
    return pl.pallas_call(
        functools.partial(gather_kernel, ns),
        out_shape=jax.ShapeDtypeStruct((ns,) + block.shape, block.dtype),
        in_specs=[any_spec],
        out_specs=any_spec,
        scratch_shapes=[dma((ns,))] * 4 + [dma],
        compiler_params=pltpu.CompilerParams(collective_id=2, has_side_effects=True),
    )(block)


def shards(
    moe_in,
    out_grad,
    expert_ids,
    route_weights,
    gate_proj,
    up_proj,
    down_proj,
    out_proj,
    conv_out,
    conv_taps,
):
    tokens, model_width = moe_in.shape
    top = expert_ids.shape[1]
    ns, nt = lax.axis_size("sp"), lax.axis_size("tp")
    ny = nt // 2
    sp, tp = lax.axis_index("sp"), lax.axis_index("tp")
    core = lax.rem(tp, 2)
    cap = -(-2 * tokens * top // ns // 16) * 16
    width = out_proj.shape[0]
    half = model_width // 2
    bf16, f32 = jnp.bfloat16, jnp.float32
    steps = jnp.arange(ns, dtype=jnp.int32)

    before = (
        jnp.arange(tokens)[:, None] > jnp.arange(tokens)[None, :]
    ).astype(bf16)

    def slots_of(experts):
        named = expert_ids[:, :, None] == experts[None, None, :]
        any_named = jnp.any(named, axis=1)
        rank = jnp.dot(before, any_named.astype(bf16), preferred_element_type=f32)
        rank = jnp.where(any_named, rank.astype(jnp.int32), -1)
        weight = jnp.sum(jnp.where(named, route_weights[:, :, None], 0.0), axis=1)
        chosen = rank.T[:, None, :] == jnp.arange(cap, dtype=jnp.int32)[None, :, None]
        return chosen, weight

    w_gate, w_up = gate_proj[0], up_proj[0]
    rows_x, rows_g, hidden, d_a, d_b = experts(
        moe_in, out_grad, expert_ids, route_weights, w_gate, w_up, down_proj[0], ns, nt, cap
    )
    act = jax.nn.silu(conv_out.astype(f32)).astype(bf16)
    send_act = act.reshape(tokens, ns, model_width // ns).transpose(1, 0, 2)
    act_all = lax.all_to_all(send_act, "sp", 0, 0)

    swap = [(t, t ^ 1) for t in range(nt)]

    def partial_half(which):
        gate = lax.dynamic_slice_in_dim(w_gate, which * half, half, 0)
        up = lax.dynamic_slice_in_dim(w_up, which * half, half, 0)
        return contract_cols(d_a, gate) + contract_cols(d_b, up)

    from_other = lax.ppermute(partial_half(1 - core).astype(bf16), "tp", swap)
    chip_sum = (partial_half(core) + from_other.astype(f32)).astype(bf16)
    chip_sum, hidden, d_a, d_b = lax.optimization_barrier((chip_sum, hidden, d_a, d_b))
    chip_sum = chip_sum.reshape(ns, cap, half)

    back = []
    for d in range(ns):
        block = lax.dynamic_index_in_dim(chip_sum, lax.rem(sp + d, ns), 0, keepdims=False)
        pair = [(s, (s + d) % ns) for s in range(ns)]
        back.append(block if d == 0 else lax.ppermute(block, "sp", pair))
    d_down = contract_rows(hidden, rows_g)
    d_gate = contract_rows(rows_x, d_a)
    d_up = contract_rows(rows_x, d_b)
    *back, d_down = lax.optimization_barrier((*back, d_down))
    back_rows = jnp.concatenate(back, axis=0)
    chosen_back, _ = slots_of(lax.rem(sp - steps + ns, ns))
    pick_back = chosen_back.reshape(ns * cap, tokens).astype(bf16)
    chip_routed = contract_rows(pick_back, back_rows).astype(bf16)
    total = chip_routed.astype(f32)
    for k in range(1, ny):
        pair = [(t, (t + 2 * k) % nt) for t in range(nt)]
        total = total + lax.ppermute(chip_routed, "tp", pair).astype(f32)
    grad_half = lax.dynamic_slice_in_dim(out_grad, core * half, half, 1).astype(f32)
    mixed_half = (grad_half + total).astype(bf16)
    mixed_other = lax.ppermute(mixed_half, "tp", swap)
    mixed_low = jnp.where(core == 0, mixed_half, mixed_other)
    mixed_high = jnp.where(core == 0, mixed_other, mixed_half)
    mixed = jnp.concatenate([mixed_low, mixed_high], axis=1)
    mixed_own = lax.dynamic_slice_in_dim(mixed, tp * width, width, 1)

    mixed_all = gather_tokens(mixed_own, ns)

    act_grad = contract_cols(mixed, out_proj)
    own_conv = lax.dynamic_slice_in_dim(conv_out, tp * width, width, 1).astype(f32)
    conv_grad = act_grad * dsilu(own_conv)
    taps = conv_taps.shape[0]
    following = lax.ppermute(
        conv_grad[: taps - 1], "sp", [(s, s - 1) for s in range(1, ns)]
    )
    extended = jnp.concatenate([conv_grad, following], axis=0)
    result = jnp.zeros((tokens, width), f32)
    for tap in range(taps):
        offset = taps - 1 - tap
        result = result + conv_taps[tap][None, :] * extended[offset : offset + tokens]

    proj_grad = contract_rows(
        act_all.reshape(ns * tokens, -1), mixed_all.reshape(ns * tokens, width)
    )
    return (d_gate[None], d_up[None], d_down[None], proj_grad, result.astype(bf16))


def solution(mesh):
    in_specs = (
        P("sp", None),
        P("sp", None),
        P("sp", None),
        P("sp", None),
        P("sp", None, "tp"),
        P("sp", None, "tp"),
        P("sp", "tp", None),
        P("tp", None),
        P("sp", None),
        P(None, "tp"),
    )
    out_specs = (
        P("sp", None, "tp"),
        P("sp", None, "tp"),
        P("sp", "tp", None),
        P("sp", "tp"),
        P("sp", "tp"),
    )
    return jax.shard_map(shards, mesh=mesh, in_specs=in_specs, out_specs=out_specs, check_vma=False)
```
